32 devices in a mesh: ep: 8 (over z, core), tp: 4 (over y, x).
Axes of the slice: x: 2, y: 2, z: 4, core: 2. Of those that a mesh axis runs over, the one named last changes fastest.
Arguments:
- branch_in: bfloat16 [8192, 512], P(('ep', 'tp')), may hold values from -6 to 6
- pool_weight: bfloat16 [4, 128, 128], replicated, may hold values from -0.5 to 0.5
- group_gain: float32 [512], replicated, may hold values from 0.1 to 1.9
- out_weight: bfloat16 [512, 2048], P(None, 'tp'), may hold values from -0.25 to 0.25
- out_gain: float32 [2048], replicated, may hold values from 0.1 to 1.9
- ffn_input: bfloat16 [1024, 2048], P('ep'), may hold values from -6 to 6
- ffn_gain: float32 [2048], replicated, may hold values from 0.1 to 1.9
- routes: int32 [1024, 4], P('ep'), may hold values from 0 to 7, all different within a row; in each aligned block of 128 rows (0 to 127, 128 to 255, ...) at most 128 rows name the same one
- route_weight: float32 [1024, 4], P('ep'), may hold values from 0.2 to 2
- gate_weight: bfloat16 [8, 2048, 4096], P('ep', None, 'tp'), may hold values from -0.375 to 0.375
- up_weight: bfloat16 [8, 2048, 4096], P('ep', None, 'tp'), may hold values from -0.375 to 0.375
- down_weight: bfloat16 [8, 4096, 2048], P('ep', 'tp'), may hold values from -0.0078125 to 0.0078125
Outputs:
- mixer_out: bfloat16 [8192, 2048], P(('ep', 'tp'))
- expert_out: bfloat16 [1024, 2048], P('ep', 'tp')
The draws below stay inside these ranges and needn't reach their ends.
Inputs may be any that keep to these rules, and one draw needn't show every extreme that they name: `routes`: each row names 4 different experts. Among the 128 rows of one index of ep no expert is named by more than 128 rows, and in some such block one expert is named by exactly 128.
All inputs are finite; a program needn't handle non-finite values.
Results may differ from the reference program's by a relative error of at most 0.017.
Values may be sent and summed in bfloat16 or wider, within the bound.
No kernel may reach another device: no remote copies, remote signals or barrier semaphores. Data moves between devices by JAX's collectives and lax.ppermute only.
A program may use at most 64 MiB of HBM per device.

```python
import math
import jax
import jax.numpy as jnp
import numpy as np
from jax import lax

D = 2048
POOL_CH = 128
GW = 512
FF = 4096
TOPK = 4
RA = 256
RB = 128
EXPERTS = 8
CAP = 128
TOKENS_A = 8192
TOKENS_B = 1024
N_EP = 8
N_TP = 4


def block_scale(rng, dims, split, least, largest):
    level = 1.0
    for axis_at, blocks in split:
        draws = jax.random.uniform(jax.random.fold_in(jax.random.fold_in(rng, 6), axis_at), (blocks,), jnp.float32, least / len(split), largest / len(split))
        level = level * jnp.repeat(jnp.exp(draws), dims[axis_at] // blocks).reshape((-1,) + (1,) * (len(dims) - 1 - axis_at))
    return level


def routed_block(stream_key, own, number, rows, amount, top, most, lean):
    ranking = jax.random.permutation(stream_key, amount)
    heavy_load, usual = shares(amount, rows * top, most, lean, True), shares(amount, rows * top, most, lean, False)
    places = jnp.arange(amount)

    def named(lengths, rotation):
        used = int((lengths > 0).sum())
        fixed = max(1, used // 4)
        passed = fixed + (places - fixed + rotation * (used - fixed)) % max(1, amount - fixed)
        return jnp.zeros((amount,), jnp.int32).at[ranking[jnp.where(places < fixed, places, passed)]].set(jnp.asarray(lengths, jnp.int32))

    lengths = jnp.where(number % 4 == 0, named(heavy_load, number // 4), named(usual, number - number // 4 - 1))
    mixed = jax.random.permutation(jax.random.fold_in(own, 3), amount)
    source_of, receiver = mixed[0:amount // 2 * 2:2], mixed[1:amount // 2 * 2:2]
    room = jnp.minimum(lengths[source_of] - 1, most - lengths[receiver]) // 2
    room = jnp.where((source_of == ranking[0]) | (receiver == ranking[0]) | (lengths[receiver] == 0), 0, jnp.maximum(room, 0))
    passed = jax.random.randint(jax.random.fold_in(own, 4), (amount // 2,), 0, 1 << 20) % (room + 1)
    lengths = lengths.at[source_of].add(-passed).at[receiver].add(passed)
    labels = jnp.searchsorted(jnp.cumsum(lengths), jnp.arange(rows * top), side="right").astype(jnp.int32)
    listing = labels.reshape(top, rows).T
    listing = listing[jax.random.permutation(jax.random.fold_in(own, 1), rows)]
    rotation = jax.random.randint(jax.random.fold_in(own, 2), (rows, 1), 0, top)
    return jnp.take_along_axis(listing, (jnp.arange(top)[None, :] + rotation) % top, axis=1)


def shares(number_of, total, limit, skew, full):
    loads = [(1 << 20) // math.isqrt(standing ** skew) + 1 for standing in range(1, number_of + 1)]
    largest = limit if full else min(limit, max(-(-total // number_of), total * loads[0] // sum(loads)))
    least = 1 if total - largest >= number_of - 1 else 0
    holding, rest = [largest] + [least] * (number_of - 1), total - largest - least * (number_of - 1)
    while rest > 0:
        candidates = [i for i in range(1, number_of) if holding[i] < largest] or [i for i in range(1, number_of) if holding[i] < limit]
        pool, remaining = sum([loads[i] for i in candidates]), rest
        for i in candidates:
            addition = min(limit - holding[i], max(1, remaining * loads[i] // pool), rest)
            holding[i] = holding[i] + addition
            rest = rest - addition
    return np.array(holding)


def scatter_about(stream_key, dims, spread, limit, pieces=(), held_as=jnp.bfloat16):
    result = jax.random.normal(stream_key, dims, jnp.float32) * spread
    if len(pieces) > 0:
        result = block_scale(stream_key, dims, pieces, -0.22, 0.18) * result
    return jnp.clip(result, min=-limit, max=limit).astype(held_as)


def setup_inputs(seed: int = 0) -> dict:
    keys = jax.random.split(jax.random.key(seed), 13)
    branch_in = scatter_about(keys[0], (TOKENS_A, GW), 1.0, 6.0, ((0, 32),))
    pool_weight = scatter_about(keys[1], (4, POOL_CH, POOL_CH), POOL_CH ** -0.5, 0.5)
    group_gain = jnp.clip(1.0 + 0.18 * jax.random.normal(keys[2], (GW,), jnp.float32), 0.1, 1.9)
    out_weight = scatter_about(keys[3], (GW, D), GW ** -0.5, 0.25, ((1, 4),))
    out_gain = jnp.clip(1.0 + 0.18 * jax.random.normal(keys[4], (D,), jnp.float32), 0.1, 1.9)
    ffn_input = scatter_about(keys[5], (TOKENS_B, D), 1.0, 6.0, ((0, 8),))
    ffn_gain = jnp.clip(1.0 + 0.18 * jax.random.normal(keys[6], (D,), jnp.float32), 0.1, 1.9)
    routes_keys = jax.random.split(jax.random.fold_in(keys[7], 1), TOKENS_B // RB)
    routes_turns = jax.random.permutation(jax.random.fold_in(keys[7], 3), TOKENS_B // RB)
    routes = jax.vmap(lambda own, number: routed_block(jax.random.fold_in(keys[7], 2), own, number, RB, EXPERTS, TOPK, CAP, 2))(routes_keys, routes_turns).reshape((TOKENS_B, TOPK))
    route_weight = jnp.clip(jnp.exp(math.log(2.0) - 2.3025851 * jax.random.uniform(keys[8], (TOKENS_B, TOPK), jnp.float32) ** block_scale(keys[8], (TOKENS_B, TOPK), ((0, 8),), -0.2, 0.2)), 0.2, 2.0)
    gate_weight = scatter_about(keys[9], (EXPERTS, D, FF), (D // 9) ** -0.5, 0.375, ((0, 8), (2, 4)))
    up_weight = scatter_about(keys[10], (EXPERTS, D, FF), (D // 9) ** -0.5, 0.375, ((0, 8), (2, 4)))
    down_weight = scatter_about(keys[11], (EXPERTS, FF, D), (FF * 160) ** -0.5, 0.0078125, ((0, 8), (1, 4)))
    return dict(branch_in=branch_in, pool_weight=pool_weight, group_gain=group_gain, out_weight=out_weight, out_gain=out_gain, ffn_input=ffn_input, ffn_gain=ffn_gain, routes=routes, route_weight=route_weight, gate_weight=gate_weight, up_weight=up_weight, down_weight=down_weight)


pool_windows = (2, 4, 8, 16)
rim_rows = 15
norm_eps = 1e-06
clamp_limit = 7.0
sigmoid_slope = 1.702

def rms_scale(values, gain):
    return values * lax.rsqrt(lax.optimization_barrier(jnp.mean(values * values, axis=-1, keepdims=True)) + norm_eps) * gain.astype(jnp.float32)

def slot_tables(route_block, expert_count, capacity):
    row_count, top_count = route_block.shape
    flat_experts = route_block.reshape(-1)
    one_hot = (flat_experts[:, None] == jnp.arange(expert_count, dtype=jnp.int32)[None, :]).astype(jnp.int32)
    earlier = jnp.cumsum(one_hot, axis=0) - one_hot
    slot_index = lax.optimization_barrier(jnp.sum(earlier * one_hot, axis=1))
    flat_slots = (slot_index * expert_count + flat_experts).astype(jnp.int32)
    owner_rows = jnp.full((capacity * expert_count,), row_count, jnp.int32)
    owner_rows = owner_rows.at[flat_slots].set(jnp.arange(row_count * top_count, dtype=jnp.int32) // top_count)
    return (flat_slots, owner_rows)

def pool_reference(branch_in, pool_weight, group_gain, out_weight, out_gain):
    total_rows, width = branch_in.shape
    group_chans = width // len(pool_windows)
    widened = jnp.concatenate([jnp.zeros((rim_rows, width), jnp.bfloat16), branch_in], axis=0)
    window = jnp.repeat(jnp.array(pool_windows, jnp.int32), group_chans)

    def one_block(block_index):
        first_row = (block_index * RA).astype(jnp.int32)
        segment = lax.dynamic_slice_in_dim(widened, first_row, RA + rim_rows, 0).astype(jnp.float32)
        positions = first_row + jnp.arange(RA, dtype=jnp.int32)
        summed = jnp.zeros((RA, width), jnp.float32)
        for offset_back in range(rim_rows + 1):
            shifted = segment[rim_rows - offset_back:rim_rows - offset_back + RA]
            summed = summed + jnp.where(window[None, :] > offset_back, shifted, jnp.float32(0.0))
        counts = jnp.minimum(window[None, :], positions[:, None] + 1).astype(jnp.float32)
        pooled = (summed / counts - segment[rim_rows:]).astype(jnp.bfloat16)
        mixed_parts = []
        for group_index in range(len(pool_windows)):
            lower = group_index * group_chans
            mixed_parts.append(jnp.dot(pooled[:, lower:lower + group_chans], pool_weight[group_index], preferred_element_type=jnp.float32))
        group_mix = jnp.concatenate(mixed_parts, axis=1)
        mixed_rows = rms_scale(group_mix, group_gain).astype(jnp.bfloat16)
        projected = jnp.dot(mixed_rows, out_weight, preferred_element_type=jnp.float32)
        return rms_scale(projected, out_gain).astype(jnp.bfloat16)
    blocks = lax.map(one_block, jnp.arange(total_rows // RA, dtype=jnp.int32))
    return blocks.reshape(total_rows, out_weight.shape[1])

def expert_reference(ffn_input, ffn_gain, routes, route_weight, gate_weight, up_weight, down_weight):
    total_rows, model_width = ffn_input.shape
    top_count = routes.shape[1]
    expert_count = gate_weight.shape[0]
    hidden_width = gate_weight.shape[2]
    row_count = total_rows // N_EP
    capacity = 2 * row_count * top_count // expert_count
    normed_rows = rms_scale(ffn_input.astype(jnp.float32), ffn_gain).astype(jnp.bfloat16)
    route_blocks = routes.reshape(N_EP, row_count, top_count)
    flat_slots, owner_rows = jax.vmap(lambda route_block: slot_tables(route_block, expert_count, capacity))(route_blocks)
    padded = jnp.concatenate([normed_rows.reshape(N_EP, row_count, model_width), jnp.zeros((N_EP, 1, model_width), jnp.bfloat16)], axis=1)
    slot_rows = jax.vmap(lambda block_rows, block_owner: block_rows[block_owner])(padded, owner_rows)
    slot_rows = slot_rows.reshape(N_EP, capacity, expert_count, model_width)
    by_expert = jnp.moveaxis(slot_rows, 2, 0).reshape(expert_count, N_EP * capacity, model_width)

    def one_expert(operands):
        expert_rows, gate_local, up_local, down_local = operands
        gate_pre = jnp.minimum(jnp.dot(expert_rows, gate_local, preferred_element_type=jnp.float32), clamp_limit)
        up_pre = jnp.clip(jnp.dot(expert_rows, up_local, preferred_element_type=jnp.float32), -clamp_limit, clamp_limit)
        hidden = ((up_pre + 1.0) * gate_pre * jax.nn.sigmoid(sigmoid_slope * gate_pre)).astype(jnp.bfloat16)
        block_width = hidden_width // N_TP
        part_hidden = hidden.astype(jnp.float32).reshape(expert_rows.shape[0], N_TP, block_width)
        part_down = down_local.astype(jnp.float32).reshape(N_TP, block_width, model_width)
        partials = jnp.einsum('ntf,tfd->tnd', part_hidden, part_down)
        partials = partials.astype(jnp.bfloat16).astype(jnp.float32)
        return lax.optimization_barrier(jnp.sum(partials, axis=0)).astype(jnp.bfloat16)
    results = lax.map(one_expert, (by_expert, gate_weight, up_weight, down_weight))
    results = results.reshape(expert_count, N_EP, capacity, model_width).transpose(1, 2, 0, 3)
    results = results.reshape(N_EP, capacity * expert_count, model_width)
    picked = jax.vmap(lambda block_results, block_slots: block_results[block_slots])(results, flat_slots)
    picked = picked.reshape(total_rows, top_count, model_width).astype(jnp.float32)
    return lax.optimization_barrier(jnp.sum(picked * route_weight[:, :, None], axis=1)).astype(jnp.bfloat16)

def reference(branch_in, pool_weight, group_gain, out_weight, out_gain, ffn_input, ffn_gain, routes, route_weight, gate_weight, up_weight, down_weight):
    mixer_out = pool_reference(branch_in, pool_weight, group_gain, out_weight, out_gain)
    expert_out = expert_reference(ffn_input, ffn_gain, routes, route_weight, gate_weight, up_weight, down_weight)
    return (mixer_out, expert_out)
```

```python
import jax
import jax.numpy as jnp
from jax import lax
from jax.sharding import PartitionSpec as P


pool_windows = (2, 4, 8, 16)
rim_rows = 15
norm_eps = 1e-06
clamp_limit = 7.0
sigmoid_slope = 1.702
both = ("ep", "tp")
lanes = 128


class Plan:
    def __init__(self, ep, tp):
        self.ep, self.tp, self.planes = ep, tp, ep // 2
        bits = [1 << i for i in range(tp.bit_length() - 1)]
        half = len(bits) // 2
        self.orders = (bits, bits[half:] + bits[:half])

    def route(self, target):
        pairs = []
        for z in range(self.planes):
            for c in range(2):
                for t in range(self.tp):
                    to_z, to_c, to_t = target(z, c, t)
                    pairs.append(
                        ((z * 2 + c) * self.tp + t, (to_z * 2 + to_c) * self.tp + to_t)
                    )
        return pairs

    def partner(self, block):
        return lax.ppermute(block, both, self.route(lambda z, c, t: (z, 1 - c, t)))

    def along_z(self, block, distance):
        return lax.ppermute(
            block, both, self.route(lambda z, c, t: ((z + distance) % self.planes, c, t))
        )

    def in_plane(self, block, stage):
        return lax.ppermute(
            block, both, self.route(lambda z, c, t: (z, c, t ^ self.orders[c][stage]))
        )

    def across(self, block, offset):
        return lax.ppermute(block, both, self.route(lambda z, c, t: (z, c, t ^ offset)))


def rms_scale(values, gain):
    return values * lax.rsqrt(jnp.mean(values * values, axis=-1, keepdims=True) + norm_eps) * gain


def pooled_rows(branch_in, pool_weight, group_gain):
    row_count, width = branch_in.shape
    group_chans = width // len(pool_windows)
    devices = lax.axis_size(both)
    route = [(i, i + 1) for i in range(devices - 1)]
    rim = lax.ppermute(branch_in[row_count - rim_rows - 1 :], both, route)
    widened = jnp.concatenate([rim[1:], branch_in], axis=0).astype(jnp.float32)
    first_row = (lax.axis_index("ep") * lax.axis_size("tp") + lax.axis_index("tp")) * row_count
    positions = first_row + jnp.arange(row_count, dtype=jnp.int32)
    window = jnp.repeat(jnp.array(pool_windows, jnp.int32), group_chans)
    summed = jnp.zeros((row_count, width), jnp.float32)
    for offset_back in range(rim_rows + 1):
        shifted = widened[rim_rows - offset_back : rim_rows - offset_back + row_count]
        summed = summed + jnp.where(window[None, :] > offset_back, shifted, jnp.float32(0.0))
    counts = jnp.minimum(window[None, :], positions[:, None] + 1).astype(jnp.float32)
    pooled = (summed / counts - widened[rim_rows:]).astype(jnp.bfloat16)
    mixed_parts = []
    for group_index in range(len(pool_windows)):
        lower = group_index * group_chans
        mixed_parts.append(
            jnp.dot(
                pooled[:, lower : lower + group_chans],
                pool_weight[group_index],
                preferred_element_type=jnp.float32,
            )
        )
    group_mix = jnp.concatenate(mixed_parts, axis=1)
    return rms_scale(group_mix, group_gain).astype(jnp.bfloat16)


def gathered_weight(plan, out_weight):
    rows, columns = out_weight.shape
    core = lax.axis_index("ep") % 2
    tp_index = lax.axis_index("tp")
    mine = lax.dynamic_slice_in_dim(out_weight, core * (rows // 2), rows // 2, 0)
    halves = jnp.stack([plan.across(mine, offset) for offset in range(1, plan.tp)], axis=0)
    others = plan.partner(halves)
    upper = jnp.where(core == 0, halves, others)
    lower = jnp.where(core == 0, others, halves)
    blocks = jnp.concatenate([upper, lower], axis=1)
    whole = jnp.zeros((rows, plan.tp * columns), out_weight.dtype)
    whole = lax.dynamic_update_slice_in_dim(whole, out_weight, tp_index * columns, 1)
    for offset in range(1, plan.tp):
        whole = lax.dynamic_update_slice_in_dim(
            whole, blocks[offset - 1], (tp_index ^ offset) * columns, 1
        )
    return whole


def expert_rows(rows, model_width, expert_count, gate_local, up_local, down_slots):
    tokens = rows[:, :model_width]
    tail = rows[:, model_width:].astype(jnp.float32)
    lane = jnp.arange(tail.shape[1], dtype=jnp.int32)[None, :]
    own = lax.axis_index("ep")
    weight = jnp.sum(
        jnp.where((lane == own) | (lane == own + expert_count), tail, 0.0), axis=1, keepdims=True
    )
    gate_pre = jnp.dot(tokens, gate_local, preferred_element_type=jnp.float32)
    up_pre = jnp.dot(tokens, up_local, preferred_element_type=jnp.float32)
    gate_pre = jnp.minimum(gate_pre, clamp_limit)
    up_pre = jnp.clip(up_pre, -clamp_limit, clamp_limit)
    hidden = ((up_pre + 1.0) * gate_pre * jax.nn.sigmoid(sigmoid_slope * gate_pre)).astype(
        jnp.bfloat16
    )
    partial = jnp.dot(hidden, down_slots, preferred_element_type=jnp.float32)
    return (partial * weight).astype(jnp.bfloat16)


def added(first, second):
    return (first.astype(jnp.float32) + second.astype(jnp.float32)).astype(jnp.bfloat16)


def routed_branch(plan, ffn_input, ffn_gain, routes, route_weight, gate_local, up_local, down_local):
    normed = rms_scale(ffn_input.astype(jnp.float32), ffn_gain).astype(jnp.bfloat16)
    row_count, model_width = normed.shape
    expert_count = lax.axis_size("ep")
    core = lax.axis_index("ep") % 2
    tp_index = lax.axis_index("tp")
    stages = len(plan.orders[0])

    experts = jnp.arange(expert_count, dtype=jnp.int32)
    dense = jnp.sum(
        jnp.where(routes[:, :, None] == experts[None, None, :], route_weight[:, :, None], 0.0),
        axis=1,
    )
    high = dense.astype(jnp.bfloat16)
    low = (dense - high.astype(jnp.float32)).astype(jnp.bfloat16)
    tail_width = -(-2 * expert_count // lanes) * lanes
    tail = jnp.concatenate(
        [high, low, jnp.zeros((row_count, tail_width - 2 * expert_count), jnp.bfloat16)], axis=1
    )
    rows = jnp.concatenate([normed, tail], axis=1)
    width = rows.shape[1]

    my_bits = []
    for stage in range(stages):
        bit = jnp.where(core == 0, plan.orders[0][stage], plan.orders[1][stage])
        my_bits.append((tp_index & bit) != 0)
    piece_index = sum(jnp.where(my_bits[s], 1 << s, 0) for s in range(stages))
    piece_rows = row_count // plan.tp
    piece = lax.dynamic_slice_in_dim(rows, piece_index * piece_rows, piece_rows, 0)

    other = plan.partner(rows)
    current = jnp.stack([plan.along_z(piece, k) for k in range(1, plan.planes)], axis=0)
    for stage in range(stages):
        received = plan.in_plane(current, stage)
        current = jnp.where(
            my_bits[stage],
            jnp.concatenate([received, current], axis=1),
            jnp.concatenate([current, received], axis=1),
        )
    far_other = plan.partner(current)
    far_rows = (plan.planes - 1) * row_count

    columns = model_width // plan.tp

    def slots_of(core_index):
        slot_blocks = []
        for slot in range(plan.tp):
            offsets = [
                sum(plan.orders[c][s] for s in range(stages) if slot & (1 << s)) for c in range(2)
            ]
            block = tp_index ^ jnp.where(core_index == 0, offsets[0], offsets[1])
            slot_blocks.append(lax.dynamic_slice_in_dim(down_local, block * columns, columns, 1))
        return jnp.concatenate(slot_blocks, axis=1)

    def run(near_rows, far_block, core_index):
        block = jnp.concatenate([near_rows, far_block.reshape(far_rows, width)], axis=0)
        return expert_rows(
            block, model_width, expert_count, gate_local, up_local, slots_of(core_index)
        )

    mine = run(rows, current, core)
    others = run(other, far_other, 1 - core)
    summed = added(mine, plan.partner(others))
    for stage in range(stages):
        half = summed.shape[1] // 2
        arrived = plan.in_plane(summed[:, half:], stages - 1 - stage)
        summed = added(summed[:, :half], arrived)
    summed = summed.reshape(plan.planes, row_count, columns)
    total = summed[0].astype(jnp.float32)
    for k in range(1, plan.planes):
        total = total + plan.along_z(summed[k], -k).astype(jnp.float32)
    return total.astype(jnp.bfloat16)


def solution(mesh):
    plan = Plan(mesh.shape["ep"], mesh.shape["tp"])

    def per_device(
        branch_in,
        pool_weight,
        group_gain,
        out_weight,
        out_gain,
        ffn_input,
        ffn_gain,
        routes,
        route_weight,
        gate_weight,
        up_weight,
        down_weight,
    ):
        expert_out = routed_branch(
            plan,
            ffn_input,
            ffn_gain,
            routes,
            route_weight,
            gate_weight[0],
            up_weight[0],
            down_weight[0],
        )
        mixed = pooled_rows(branch_in, pool_weight, group_gain)
        projected = jnp.dot(
            mixed, gathered_weight(plan, out_weight), preferred_element_type=jnp.float32
        )
        return (rms_scale(projected, out_gain).astype(jnp.bfloat16), expert_out)

    in_specs = (
        P(("ep", "tp"), None),
        P(),
        P(),
        P(None, "tp"),
        P(),
        P("ep", None),
        P(),
        P("ep", None),
        P("ep", None),
        P("ep", None, "tp"),
        P("ep", None, "tp"),
        P("ep", "tp", None),
    )
    out_specs = (P(("ep", "tp"), None), P("ep", "tp"))
    return jax.shard_map(
        per_device, mesh=mesh, in_specs=in_specs, out_specs=out_specs, check_vma=False
    )
```

```python
import functools

import jax
import jax.numpy as jnp
from jax import lax
from jax.experimental import pallas as pl
from jax.experimental.pallas import tpu as pltpu
from jax.sharding import PartitionSpec as P


pool_windows = (2, 4, 8, 16)
rim_rows = 15
norm_eps = 1e-06
clamp_limit = 7.0
sigmoid_slope = 1.702
both = ("ep", "tp")
lanes = 128


class Plan:
    def __init__(self, ep, tp):
        self.ep, self.tp, self.planes = ep, tp, ep // 2
        bits = [1 << i for i in range(tp.bit_length() - 1)]
        half = len(bits) // 2
        self.orders = (bits, bits[half:] + bits[:half])

    def route(self, target):
        pairs = []
        for z in range(self.planes):
            for c in range(2):
                for t in range(self.tp):
                    to_z, to_c, to_t = target(z, c, t)
                    pairs.append(
                        ((z * 2 + c) * self.tp + t, (to_z * 2 + to_c) * self.tp + to_t)
                    )
        return pairs

    def partner(self, block):
        return lax.ppermute(block, both, self.route(lambda z, c, t: (z, 1 - c, t)))

    def along_z(self, block, distance):
        return lax.ppermute(
            block, both, self.route(lambda z, c, t: ((z + distance) % self.planes, c, t))
        )

    def in_plane(self, block, stage):
        return lax.ppermute(
            block, both, self.route(lambda z, c, t: (z, c, t ^ self.orders[c][stage]))
        )

    def across(self, block, offset):
        return lax.ppermute(block, both, self.route(lambda z, c, t: (z, c, t ^ offset)))


def rms_scale(values, gain):
    return values * lax.rsqrt(jnp.mean(values * values, axis=-1, keepdims=True) + norm_eps) * gain


def pooled_rows(branch_in, pool_weight, group_gain):
    row_count, width = branch_in.shape
    group_chans = width // len(pool_windows)
    devices = lax.axis_size(both)
    route = [(i, i + 1) for i in range(devices - 1)]
    rim = lax.ppermute(branch_in[row_count - rim_rows - 1 :], both, route)
    widened = jnp.concatenate([rim[1:], branch_in], axis=0).astype(jnp.float32)
    first_row = (lax.axis_index("ep") * lax.axis_size("tp") + lax.axis_index("tp")) * row_count
    positions = first_row + jnp.arange(row_count, dtype=jnp.int32)
    window = jnp.repeat(jnp.array(pool_windows, jnp.int32), group_chans)
    summed = jnp.zeros((row_count, width), jnp.float32)
    for offset_back in range(rim_rows + 1):
        shifted = widened[rim_rows - offset_back : rim_rows - offset_back + row_count]
        summed = summed + jnp.where(window[None, :] > offset_back, shifted, jnp.float32(0.0))
    counts = jnp.minimum(window[None, :], positions[:, None] + 1).astype(jnp.float32)
    pooled = (summed / counts - widened[rim_rows:]).astype(jnp.bfloat16)
    mixed_parts = []
    for group_index in range(len(pool_windows)):
        lower = group_index * group_chans
        mixed_parts.append(
            jnp.dot(
                pooled[:, lower : lower + group_chans],
                pool_weight[group_index],
                preferred_element_type=jnp.float32,
            )
        )
    group_mix = jnp.concatenate(mixed_parts, axis=1)
    return rms_scale(group_mix, group_gain).astype(jnp.bfloat16)


def gathered_weight(plan, out_weight):
    rows, columns = out_weight.shape
    core = lax.axis_index("ep") % 2
    tp_index = lax.axis_index("tp")
    mine = lax.dynamic_slice_in_dim(out_weight, core * (rows // 2), rows // 2, 0)
    halves = jnp.stack([plan.across(mine, offset) for offset in range(1, plan.tp)], axis=0)
    others = plan.partner(halves)
    upper = jnp.where(core == 0, halves, others)
    lower = jnp.where(core == 0, others, halves)
    blocks = jnp.concatenate([upper, lower], axis=1)
    whole = jnp.zeros((rows, plan.tp * columns), out_weight.dtype)
    whole = lax.dynamic_update_slice_in_dim(whole, out_weight, tp_index * columns, 1)
    for offset in range(1, plan.tp):
        whole = lax.dynamic_update_slice_in_dim(
            whole, blocks[offset - 1], (tp_index ^ offset) * columns, 1
        )
    return whole


def prologue_kernel(tokens, gain, routes, route_weight, out, *, experts):
    depth = tokens.shape[1]
    values = tokens[...].astype(jnp.float32)
    scale = lax.rsqrt(jnp.mean(values * values, axis=1, keepdims=True) + norm_eps)
    out[:, :depth] = (values * scale * gain[...]).astype(jnp.bfloat16)
    count, tail_width = out.shape[0], out.shape[1] - depth
    lane = lax.broadcasted_iota(jnp.int32, (count, tail_width), 1)
    expert = jnp.where(lane < experts, lane, lane - experts)
    dense = jnp.zeros((count, tail_width), jnp.float32)
    for k in range(routes.shape[1]):
        dense = dense + jnp.where(routes[:, k : k + 1] == expert, route_weight[:, k : k + 1], 0.0)
    high = dense.astype(jnp.bfloat16).astype(jnp.float32)
    tail = jnp.where(lane < experts, high, dense - high)
    out[:, depth:] = jnp.where(lane < 2 * experts, tail, 0.0).astype(jnp.bfloat16)


def prologue(ffn_input, ffn_gain, routes, route_weight, experts):
    count, depth = ffn_input.shape
    tail_width = -(-2 * experts // lanes) * lanes
    in_vmem = pl.BlockSpec(memory_space=pltpu.VMEM)
    return pl.pallas_call(
        functools.partial(prologue_kernel, experts=experts),
        out_shape=jax.ShapeDtypeStruct((count, depth + tail_width), jnp.bfloat16),
        in_specs=[in_vmem] * 4,
        out_specs=in_vmem,
        compiler_params=pltpu.CompilerParams(vmem_limit_bytes=8 << 20),
        cost_estimate=pl.CostEstimate(
            flops=8 * count * depth, bytes_accessed=4 * count * depth, transcendentals=0
        ),
    )(ffn_input, ffn_gain.reshape(1, depth), routes, route_weight)


def expert_kernel(meta, *refs, layout, planes, tile, slots, experts):
    blocks = refs[: len(layout)]
    gate, up, down, out_mine, out_other, rows, weights, hidden = refs[len(layout) :]
    depth, units = gate.shape
    count = out_mine.shape[0]
    per_plane = count // planes
    own = meta[0]
    for ref, (side, half) in zip(blocks, layout):
        height = ref.shape[0] // planes
        for g in range(planes):
            base = side * count + g * per_plane
            if half is not None:
                bit = meta[1 + side]
                base = base + (bit if half == 0 else 1 - bit) * height
                base = pl.multiple_of(base, height)
            block = ref[g * height : (g + 1) * height, :]
            rows[pl.ds(base, height), :] = block[:, :depth]
            tail = block[:, depth:].astype(jnp.float32)
            lane = lax.broadcasted_iota(jnp.int32, tail.shape, 1)
            chosen = (lane == own) | (lane == own + experts)
            weights[pl.ds(base, height), :] = jnp.sum(
                jnp.where(chosen, tail, 0.0), axis=1, keepdims=True
            )

    @pl.loop(0, units // tile)
    def _(step):
        at = pl.ds(pl.multiple_of(step * tile, tile), tile)
        gate_pre = jnp.dot(rows[...], gate[:, at], preferred_element_type=jnp.float32)
        up_pre = jnp.dot(rows[...], up[:, at], preferred_element_type=jnp.float32)
        gate_pre = jnp.minimum(gate_pre, clamp_limit)
        up_pre = jnp.clip(up_pre, -clamp_limit, clamp_limit)
        value = (up_pre + 1.0) * gate_pre * jax.nn.sigmoid(sigmoid_slope * gate_pre)
        hidden[:, at] = value.astype(jnp.bfloat16)

    columns = down.shape[1] // slots

    @pl.loop(0, slots)
    def _(block):
        at = pl.ds(pl.multiple_of(block * columns, columns), columns)
        partial = jnp.dot(hidden[...], down[:, at], preferred_element_type=jnp.float32)
        partial = (partial * weights[...]).astype(jnp.bfloat16)
        first = meta[3 + block]
        second = meta[3 + slots + block]
        out_mine[:, pl.ds(pl.multiple_of(first * columns, columns), columns)] = partial[:count]
        out_other[:, pl.ds(pl.multiple_of(second * columns, columns), columns)] = partial[count:]


def expert_call(meta, blocks, layout, planes, count, gate, up, down, experts, slots):
    depth, units = gate.shape
    in_vmem = pl.BlockSpec(memory_space=pltpu.VMEM)
    kernel = functools.partial(
        expert_kernel,
        layout=layout,
        planes=planes,
        tile=min(256, units),
        slots=slots,
        experts=experts,
    )
    return pl.pallas_call(
        kernel,
        out_shape=[jax.ShapeDtypeStruct((count, down.shape[1]), jnp.bfloat16)] * 2,
        in_specs=[pl.BlockSpec(memory_space=pltpu.SMEM)] + [in_vmem] * (len(blocks) + 3),
        out_specs=[in_vmem] * 2,
        scratch_shapes=[
            pltpu.VMEM((2 * count, depth), jnp.bfloat16),
            pltpu.VMEM((2 * count, 1), jnp.float32),
            pltpu.VMEM((2 * count, units), jnp.bfloat16),
        ],
        compiler_params=pltpu.CompilerParams(vmem_limit_bytes=30 << 20),
        cost_estimate=pl.CostEstimate(
            flops=12 * count * depth * units, bytes_accessed=6 * depth * units, transcendentals=0
        ),
    )(meta, *blocks, gate, up, down)


def added(first, second):
    return (first.astype(jnp.float32) + second.astype(jnp.float32)).astype(jnp.bfloat16)


def routed_branch(plan, ffn_input, ffn_gain, routes, route_weight, gate_local, up_local, down_local):
    expert_count = lax.axis_size("ep")
    rows = prologue(ffn_input, ffn_gain, routes, route_weight, expert_count)
    row_count, width = rows.shape
    model_width = ffn_input.shape[1]
    own = lax.axis_index("ep")
    core = own % 2
    tp_index = lax.axis_index("tp")
    stages = len(plan.orders[0])

    def bit_of(core_index, stage):
        bit = jnp.where(core_index == 0, plan.orders[0][stage], plan.orders[1][stage])
        return (tp_index & bit) != 0

    my_bits = [bit_of(core, stage) for stage in range(stages)]
    piece_index = sum(jnp.where(my_bits[s], 1 << s, 0) for s in range(stages))
    piece_rows = row_count // plan.tp
    piece = lax.dynamic_slice_in_dim(rows, piece_index * piece_rows, piece_rows, 0)

    meta = [own, my_bits[-1].astype(jnp.int32), bit_of(1 - core, stages - 1).astype(jnp.int32)]
    for core_index in (core, 1 - core):
        offset_of = [
            sum(jnp.where(core_index == c, plan.orders[c][s], 0) for c in range(2))
            for s in range(stages)
        ]
        for block in range(plan.tp):
            difference = tp_index ^ block
            meta.append(
                sum(jnp.where((difference & offset_of[s]) != 0, 1 << s, 0) for s in range(stages))
            )
    meta = jnp.stack(meta).astype(jnp.int32)

    def run(blocks, layout, planes):
        count = planes * row_count
        return expert_call(
            meta,
            blocks,
            layout,
            planes,
            count,
            gate_local,
            up_local,
            down_local,
            expert_count,
            plan.tp,
        )

    def combine(mine, other):
        arrived = plan.partner(other)
        for stage in range(stages):
            half = mine.shape[1] // 2
            if stage == 0:
                sent = added(mine[:, half:], arrived[:, half:])
                kept = added(mine[:, :half], arrived[:, :half])
            else:
                sent = added(kept_mine[:, half:], kept_arrived[:, half:])
                kept = added(kept_mine[:, :half], kept_arrived[:, :half])
            kept_arrived = plan.in_plane(sent, stages - 1 - stage)
            kept_mine = kept
            mine = kept
        return kept_mine, kept_arrived

    near = combine(*run([rows, plan.partner(rows)], ((0, None), (1, None)), 1))
    total = near[0].astype(jnp.float32) + near[1].astype(jnp.float32)

    distances = sorted(range(1, plan.planes), key=lambda k: (min(k, plan.planes - k), k))
    groups = [distances[i : i + 2] for i in range(0, len(distances), 2)]
    arrivals = {k: plan.along_z(piece, k) for k in distances}
    for group in groups:
        planes = len(group)
        current = jnp.stack([arrivals[k] for k in group], axis=0)
        for stage in range(stages):
            received = plan.in_plane(current, stage)
            if stage == stages - 1:
                break
            current = jnp.where(
                my_bits[stage],
                jnp.concatenate([received, current], axis=1),
                jnp.concatenate([current, received], axis=1),
            )
        current = current.reshape(-1, width)
        received = received.reshape(-1, width)
        blocks = [current, received, plan.partner(current), plan.partner(received)]
        mine, other = run(blocks, ((0, 0), (0, 1), (1, 0), (1, 1)), planes)
        kept, arrived = combine(mine, other)
        summed = added(kept, arrived)
        for i, k in enumerate(group):
            home = plan.along_z(summed[i * row_count : (i + 1) * row_count], -k)
            total = total + home.astype(jnp.float32)
    return total.astype(jnp.bfloat16)


def solution(mesh):
    plan = Plan(mesh.shape["ep"], mesh.shape["tp"])

    def per_device(
        branch_in,
        pool_weight,
        group_gain,
        out_weight,
        out_gain,
        ffn_input,
        ffn_gain,
        routes,
        route_weight,
        gate_weight,
        up_weight,
        down_weight,
    ):
        expert_out = routed_branch(
            plan,
            ffn_input,
            ffn_gain,
            routes,
            route_weight,
            gate_weight[0],
            up_weight[0],
            down_weight[0],
        )
        mixed = pooled_rows(branch_in, pool_weight, group_gain)
        projected = jnp.dot(
            mixed, gathered_weight(plan, out_weight), preferred_element_type=jnp.float32
        )
        return (rms_scale(projected, out_gain).astype(jnp.bfloat16), expert_out)

    in_specs = (
        P(("ep", "tp"), None),
        P(),
        P(),
        P(None, "tp"),
        P(),
        P("ep", None),
        P(),
        P("ep", None),
        P("ep", None),
        P("ep", None, "tp"),
        P("ep", None, "tp"),
        P("ep", "tp", None),
    )
    out_specs = (P(("ep", "tp"), None), P("ep", "tp"))
    return jax.shard_map(
        per_device, mesh=mesh, in_specs=in_specs, out_specs=out_specs, check_vma=False
    )
```
